32 devices in a mesh: ep: 8 (over z, y), tp: 4 (over x, core).
Axes of the slice: x: 2, y: 2, z: 4, core: 2. Of those that a mesh axis runs over, the one named last changes fastest.
Arguments:
- tokens: bfloat16 [2048, 2048], P('ep', 'tp'), may hold values from -400 to 400
- expert_ids: int32 [2048, 2], P('ep'), may hold values from 0 to 7, all different within a row; in each aligned block of 256 rows (0 to 255, 256 to 511, ...) at most 80 rows name the same one
- route_weights: float32 [2048, 2], P('ep'), may hold values from 0.1 to 1
- pre_gain: float32 [2048], P('tp'), may hold values from 0.1 to 1.9
- post_gain: float32 [2048], P('tp'), may hold values from 0.1 to 1.9
- gate_weight: bfloat16 [8, 2048, 4096], P('ep', None, 'tp'), may hold values from -0.125 to 0.125
- up_weight: bfloat16 [8, 2048, 4096], P('ep', None, 'tp'), may hold values from -0.125 to 0.125
- down_weight: bfloat16 [8, 4096, 2048], P('ep', None, 'tp'), may hold values from -0.71875 to 0.71875
Outputs:
- layer_out: bfloat16 [2048, 2048], P('ep', 'tp')
The draws below stay inside these ranges and needn't reach their ends.
Inputs may be any that keep to these rules, and one draw needn't show every extreme that they name: `expert_ids`: the 2 experts of a token are distinct. Within the rows of one device along ep, no expert is named more than 80 times, a bound that some block reaches.
All inputs are finite; a program needn't handle non-finite values.
Results may differ from the reference program's by a relative error of at most 0.007.
Values may be sent and summed in bfloat16 or wider, within the bound.
A program may use at most 64 MiB of HBM per device.

```python
import math
import jax
import jax.numpy as jnp
import numpy as np
from jax import lax

D = 2048
DE = 4096
TOPK = 2
TOK_DEV = 256
EXPERTS = 8
TOKENS = 2048
CAP = 80
N_EP = 8


def draw_tokens(key, part):
    first, second, third = jax.random.split(jax.random.fold_in(key, 11), 3)
    base = jnp.clip(jax.random.normal(first, (TOKENS, D), jnp.float32), -6.0, 6.0)
    rising = jnp.exp(jnp.log(4.0) * jnp.arange(D, dtype=jnp.float32) / D)
    rough = jax.random.uniform(second, (1, D), jnp.float32, 0.5, 1.5)
    row_scale = jnp.exp(jax.random.uniform(third, (TOKENS, 1), jnp.float32, 0.0, jnp.log(10.0)))
    return (base * rising[None, :] * rough * row_scale).astype(jnp.bfloat16)


def draw_down_weight(key, part):
    first, second = jax.random.split(jax.random.fold_in(key, 23), 2)
    base = jnp.clip(jax.random.normal(first, (EXPERTS, DE, D), jnp.float32), -6.0, 6.0)
    rising = jnp.exp(jnp.log(5.0) * jnp.arange(D, dtype=jnp.float32) / D)
    rough = jax.random.uniform(second, (1, 1, D), jnp.float32, 0.5, 1.5)
    return (base * rising[None, None, :] * rough * DE ** (-0.5)).astype(jnp.bfloat16)


def steps_of(stream_key, dims, cuts, smallest, top_value):
    level, own = 1.0, jax.random.fold_in(stream_key, 6)
    for axis_at, parts in cuts:
        steps = jnp.exp(jax.random.uniform(jax.random.fold_in(own, axis_at), (parts,), jnp.float32, smallest / len(cuts), top_value / len(cuts)))
        level = level * jnp.repeat(steps, dims[axis_at] // parts).reshape([-1 if axis == axis_at else 1 for axis in range(len(dims))])
    return level


def assign_block(key, own, number, rows, count, top, reach, skew):
    order = jax.random.permutation(key, count)
    packed, common = load_shares(count, rows * top, reach, skew, True), load_shares(count, rows * top, reach, skew, False)
    places = jnp.arange(count)

    def named(tallies, turn):
        used = int((tallies > 0).sum())
        fixed = max(1, used // 4)
        moved = fixed + (places - fixed + turn * (used - fixed)) % max(1, count - fixed)
        return jnp.zeros((count,), jnp.int32).at[order[jnp.where(places < fixed, places, moved)]].set(jnp.asarray(tallies, jnp.int32))

    tallies = jnp.where(number % 4 == 0, named(packed, number // 4), named(common, number - number // 4 - 1))
    mixed = jax.random.permutation(jax.random.fold_in(own, 3), count)
    giver, receiver = mixed[0:count // 2 * 2:2], mixed[1:count // 2 * 2:2]
    margin = jnp.minimum(tallies[giver] - 1, reach - tallies[receiver]) // 2
    margin = jnp.where((giver == order[0]) | (receiver == order[0]) | (tallies[receiver] == 0), 0, jnp.maximum(margin, 0))
    moved = jax.random.randint(jax.random.fold_in(own, 4), (count // 2,), 0, 1 << 20) % (margin + 1)
    tallies = tallies.at[giver].add(-moved).at[receiver].add(moved)
    items = jnp.searchsorted(jnp.cumsum(tallies), jnp.arange(rows * top), side="right").astype(jnp.int32)
    grid = items.reshape(top, rows).T
    grid = grid[jax.random.permutation(jax.random.fold_in(own, 1), rows)]
    turn = jax.random.randint(jax.random.fold_in(own, 2), (rows, 1), 0, top)
    return jnp.take_along_axis(grid, (jnp.arange(top)[None, :] + turn) % top, axis=1)


def load_shares(count, total, bound, skew, full):
    portions = [(1 << 20) // math.isqrt(standing ** skew) + 1 for standing in range(1, count + 1)]
    largest = bound if full else min(bound, max(-(-total // count), total * portions[0] // sum(portions)))
    least = 1 if total - largest >= count - 1 else 0
    given, spare = [largest] + [least] * (count - 1), total - largest - least * (count - 1)
    while spare > 0:
        free = [i for i in range(1, count) if given[i] < largest] or [i for i in range(1, count) if given[i] < bound]
        mass, remaining = sum([portions[i] for i in free]), spare
        for i in free:
            addition = min(bound - given[i], max(1, remaining * portions[i] // mass), spare)
            given[i] = given[i] + addition
            spare = spare - addition
    return np.array(given)


def bell_draw(own_key, extent, width, most, cuts=(), kind=jnp.bfloat16):
    result = width * jax.random.normal(own_key, extent, jnp.float32)
    if cuts:
        result = result * steps_of(own_key, extent, cuts, -0.22, 0.18)
    return jnp.clip(result, -most, most).astype(kind)


def setup_inputs(seed: int = 0) -> dict:
    streams_of = jax.random.split(jax.random.key(seed), 9)
    tokens = draw_tokens(jax.random.fold_in(streams_of[8], 71), 0)
    expert_ids_keys = jax.random.split(jax.random.fold_in(streams_of[1], 1), TOKENS // TOK_DEV)
    expert_ids_turns = jax.random.permutation(jax.random.fold_in(streams_of[1], 3), TOKENS // TOK_DEV)
    expert_ids = jax.vmap(lambda own, number: assign_block(jax.random.fold_in(streams_of[1], 2), own, number, TOK_DEV, EXPERTS, TOPK, CAP, 2))(expert_ids_keys, expert_ids_turns).reshape((TOKENS, TOPK))
    route_weights = jnp.clip(0.1 + 0.9 * jax.random.uniform(streams_of[2], (TOKENS, TOPK), jnp.float32) ** steps_of(streams_of[2], (TOKENS, TOPK), ((0, 8),), -0.2, 0.2), 0.1, 1.0)
    pre_gain = jnp.clip(1.0 + 0.18 * jax.random.normal(streams_of[3], (D,), jnp.float32), 0.1, 1.9)
    post_gain = jnp.clip(1.0 + 0.18 * jax.random.normal(streams_of[4], (D,), jnp.float32), 0.1, 1.9)
    gate_weight = bell_draw(streams_of[5], (EXPERTS, D, DE), D ** -0.5, 0.125, ((0, 8), (2, 4)))
    up_weight = bell_draw(streams_of[6], (EXPERTS, D, DE), D ** -0.5, 0.125, ((0, 8), (2, 4)))
    down_weight = draw_down_weight(jax.random.fold_in(streams_of[8], 71), 0)
    return {"tokens": tokens, "expert_ids": expert_ids, "route_weights": route_weights, "pre_gain": pre_gain, "post_gain": post_gain, "gate_weight": gate_weight, "up_weight": up_weight, "down_weight": down_weight}


epsilon = 1e-06

def reference(tokens, expert_ids, route_weights, pre_gain, post_gain, gate_weight, up_weight, down_weight):
    tok_float = tokens.astype(jnp.float32)
    mean_in = lax.optimization_barrier(jnp.mean(tok_float * tok_float, axis=1, keepdims=True))
    normed = (tok_float * lax.rsqrt(mean_in + epsilon) * pre_gain.astype(jnp.float32)[None, :]).astype(jnp.bfloat16)
    pairs = N_EP * TOK_DEV * TOPK
    blocks = expert_ids.reshape(N_EP, TOK_DEV * TOPK)
    onehot = (blocks[:, :, None] == jnp.arange(EXPERTS, dtype=jnp.int32)[None, None, :]).astype(jnp.int32)
    slot = lax.optimization_barrier(jnp.sum((jnp.cumsum(onehot, axis=1) - 1) * onehot, axis=2)).astype(jnp.int32).reshape(-1)
    block_of = jnp.arange(pairs, dtype=jnp.int32) // (TOK_DEV * TOPK)
    flat_ids = expert_ids.reshape(-1).astype(jnp.int32)
    row_of = (block_of * CAP + slot).astype(jnp.int32)
    token_of = jnp.arange(pairs, dtype=jnp.int32) // TOPK
    table = jnp.full((EXPERTS, N_EP * CAP), TOKENS, jnp.int32).at[flat_ids, row_of].set(token_of)
    padded = jnp.concatenate([normed, jnp.zeros((1, D), jnp.bfloat16)], axis=0)

    def expert(inputs):
        row_index, w_gate, w_up, w_down = inputs
        rows = padded[row_index].astype(jnp.float32)
        gate = jnp.dot(rows, w_gate.astype(jnp.float32))
        upper = jnp.dot(rows, w_up.astype(jnp.float32))
        hidden = (jax.nn.silu(gate) * upper).astype(jnp.bfloat16)
        return jnp.dot(hidden.astype(jnp.float32), w_down.astype(jnp.float32)).astype(jnp.bfloat16)
    results = lax.map(expert, (table, gate_weight, up_weight, down_weight))
    picked = results[flat_ids, row_of].reshape(TOKENS, TOPK, D).astype(jnp.float32)
    mixed = lax.optimization_barrier(jnp.sum(picked * route_weights.astype(jnp.float32)[:, :, None], axis=1))
    mean_out = lax.optimization_barrier(jnp.mean(mixed * mixed, axis=1, keepdims=True))
    return (mixed * lax.rsqrt(mean_out + epsilon) * post_gain.astype(jnp.float32)[None, :]).astype(jnp.bfloat16)
```

```python
import functools

import jax
import jax.numpy as jnp
from jax import lax
from jax.experimental import pallas as pl
from jax.experimental.pallas import tpu as pltpu
from jax.sharding import PartitionSpec as P

epsilon = 1e-06
MESH = pl.DeviceIdType.MESH
f32, bf16 = jnp.float32, jnp.bfloat16


def flip(index, bits):
    out, bit = index, 1
    while bit <= bits:
        if bits & bit:
            out = out + bit * (1 - 2 * ((index // bit) % 2))
        bit *= 2
    return out


def to_column(row):
    return jnp.transpose(jnp.broadcast_to(row, (128, row.shape[1])))


def wide(column, width):
    return jnp.concatenate([column] * (width // 128), axis=1)


def row_sums(values):
    part = values[:, 0:128]
    for at in range(128, values.shape[1], 128):
        part = part + values[:, at : at + 128]
    return jnp.sum(jnp.transpose(part), axis=0, keepdims=True)


def kernel(
    n, tp, cap, groups, shared, early, pieces,
    tok_ref, ids_ref, rw_ref, pre_ref, post_ref, wg_hbm, wu_hbm, wd_hbm,
    out_ref,
    wg, wu, wd, tok_x, outg, feats, rows_in, hid, part, back, ret, gain, ss_out, mix, wcol, *rest,
):
    picks, sems = rest[: len(pieces)], rest[len(pieces) :]
    (w_sem, met_ep, met_tp, t_s, t_r, g_s, g_r, so_s, so_r, d_s, d_r, fx_s, fx_r, fp_s, fp_r,
     hx_s, hx_r, hp_s, hp_r, r_s, r_r) = sems
    me, ti = lax.axis_index("ep"), lax.axis_index("tp")
    chips = tp // 2
    chip, core = ti // 2, ti % 2
    partner = chip * 2 + (1 - core)
    rows, width = tok_ref.shape
    side = chips * width
    units = wg.shape[1]
    n_tile = min(256, units)
    tiles = units // n_tile
    per_group = n // groups
    group_rows = per_group * cap

    barrier = pltpu.get_barrier_semaphore()

    def signal(sem, where):
        pl.semaphore_signal(sem, inc=1, device_id=where, device_id_type=MESH)

    for j in range(1, tp):
        peer = (ti + j) % tp
        pl.when(peer > ti)(functools.partial(signal, barrier, {"tp": peer}))
    for d in range(1, n):
        peer = flip(me, d)
        pl.when(peer > me)(functools.partial(signal, barrier, {"ep": peer}))

    def load_all(src, dst, sem, step, place):
        for at in range(0, dst.shape[0], step):
            pltpu.make_async_copy(
                src.at[0, pl.ds(at, step)], dst.at[pl.ds(place(at // step) * step, step)], sem
            ).start()

    def position(owner):
        return owner % 2 * chips + owner // 2

    load_all(wg_hbm, wg, w_sem.at[0], width, position)
    load_all(wu_hbm, wu, w_sem.at[1], width, position)
    load_all(
        wd_hbm, wd, w_sem.at[2], n_tile, lambda at: at % tiles * tp + position(at // tiles)
    )
    loads = [
        pltpu.make_async_copy(src.at[0], dst, w_sem.at[i])
        for i, (src, dst) in enumerate(((wg_hbm, wg), (wu_hbm, wu), (wd_hbm, wd)))
    ]

    pl.when(me + ti > 0)(lambda: pl.semaphore_wait(barrier, me + ti))
    for j in range(1, tp):
        peer = (ti + j) % tp
        pl.when(peer < ti)(functools.partial(signal, met_tp.at[tp - j - 1], {"tp": peer}))
    for d in range(1, n):
        peer = flip(me, d)
        pl.when(peer < me)(functools.partial(signal, met_ep.at[d - 1], {"ep": peer}))

    def meet_tp(j):
        pl.when((ti + j) % tp > ti)(lambda: pl.semaphore_wait(met_tp.at[j - 1], 1))

    def meet_ep(d):
        pl.when(flip(me, d) > me)(lambda: pl.semaphore_wait(met_ep.at[d - 1], 1))

    def remote(src, dst, s_sem, r_sem, where):
        return pltpu.make_async_remote_copy(
            src_ref=src, dst_ref=dst, send_sem=s_sem, recv_sem=r_sem,
            device_id=where, device_id_type=MESH,
        )

    lanes = max(n, 16)
    rel = [jnp.bitwise_xor(ids_ref[k : k + 1, :], me) for k in range(2)]
    d_iota = lax.broadcasted_iota(jnp.int32, (lanes, rows), 0)
    hot = [jnp.where(rel[k] == d_iota, 1.0, 0.0).astype(f32) for k in range(2)]
    earlier = jnp.where(
        lax.broadcasted_iota(jnp.int32, (rows, rows), 0)
        < lax.broadcasted_iota(jnp.int32, (rows, rows), 1), 1.0, 0.0,
    ).astype(bf16)
    prefix = jnp.dot((hot[0] + hot[1]).astype(bf16), earlier, preferred_element_type=f32)
    target = [
        rel[k].astype(f32) * cap + jnp.sum(prefix * hot[k], axis=0, keepdims=True)
        for k in range(2)
    ]
    slot_iota = lax.broadcasted_iota(jnp.int32, (cap, rows), 0).astype(f32)

    def hop(j):
        return (chip + j) % chips

    def seg(j):
        return pl.ds(pl.multiple_of(core * side + hop(j) * width, 128), width)

    def tok_seg(j):
        return pl.ds(pl.multiple_of(hop(j) * width, 128), width)

    own = seg(0)
    half = pl.ds(pl.multiple_of(core * side, 128), side)

    def block(d):
        return pl.ds(d * cap, cap)

    def group(g):
        return pl.ds(g * group_rows, group_rows)

    def members(g):
        return range(g * per_group, (g + 1) * per_group)

    def token_copy(j):
        return remote(
            tok_ref, tok_x.at[:, tok_seg(0)], t_s.at[0], t_r.at[j - 1], {"tp": hop(j) * 2 + core}
        )

    def gain_copy(j):
        return remote(pre_ref, gain.at[:, own], g_s.at[0], g_r.at[j - 1], {"tp": (ti + j) % tp})

    def dispatch_copy(d, j):
        return remote(
            outg.at[block(d), tok_seg(j)], feats.at[block(d), seg(j)],
            d_s.at[0], d_r.at[d - 1, j], {"ep": flip(me, d)},
        )

    def feat_x(g, j):
        ref = feats.at[group(g), own]
        return remote(ref, ref, fx_s.at[0], fx_r.at[g, j - 1], {"tp": hop(j) * 2 + core})

    def feat_pair(g):
        ref = feats.at[group(g), half]
        return remote(ref, ref, fp_s.at[0], fp_r.at[g], {"tp": partner})

    def choose(d, j):
        base = float(d * cap)
        chosen = jnp.where(
            (target[0] == slot_iota + base) | (target[1] == slot_iota + base), 1.0, 0.0
        ).astype(bf16)
        source = tok_ref[...] if j == 0 else tok_x[:, tok_seg(j)]
        picked = jnp.dot(chosen, source, preferred_element_type=f32).astype(bf16)
        if d == 0:
            feats[block(0), seg(j)] = picked
        else:
            outg[block(d), tok_seg(j)] = picked

    def pick_own(g):
        for d in members(g):
            choose(d, 0)

    def send_own(g):
        for d in members(g):
            if d > 0:
                meet_ep(d)
                dispatch_copy(d, 0).start()

    def send_rest(g):
        for d in members(g):
            for j in range(1, chips):
                choose(d, j)
                if d > 0:
                    dispatch_copy(d, j).start()

    def take(g):
        for d in members(g):
            for j in range(1 if g in shared else chips):
                if d > 0:
                    dispatch_copy(d, j).wait_recv()
        if g in shared:
            for j in range(1, chips):
                feat_x(g, j).start()
        else:
            feat_pair(g).start()

    def pass_on(g):
        for j in range(1, chips):
            feat_x(g, j).wait_recv()
        feat_pair(g).start()

    def tile_at(i, owner):
        return pl.multiple_of((i * tp + position(owner)) * n_tile, 128)

    def hid_x(g, i, j):
        ref = hid.at[group(g), pl.ds(tile_at(i, ti), n_tile)]
        return remote(ref, ref, hx_s.at[0], hx_r.at[g, i, j - 1], {"tp": hop(j) * 2 + core})

    def hid_pair(g, i):
        at = pl.multiple_of((i * tp + core * chips) * n_tile, 128)
        ref = hid.at[group(g), pl.ds(at, chips * n_tile)]
        return remote(ref, ref, hp_s.at[0], hp_r.at[g, i], {"tp": partner})

    def send_tile(g, i):
        for j in range(1, chips):
            hid_x(g, i, j).start()

    def send_hidden(g, first):
        for i in range(first, tiles):
            send_tile(g, i)

    def gate_up(g, sent=tiles):
        feat_pair(g).wait_recv()
        batch = max(u for u in range(1, 6) if (group_rows // 16) % u == 0)

        def norm(i, carry):
            for u in range(batch):
                here = (i * batch + u) * 16
                span = pl.ds(pl.multiple_of(g * group_rows + here, 16), 16)
                x = feats[span, :].astype(f32)
                square = jnp.sum(x * x, axis=1, keepdims=True)
                x = x * lax.rsqrt(square / (width * tp) + epsilon) * gain[...]
                rows_in[pl.ds(pl.multiple_of(here, 16), 16), :] = x.astype(bf16)
            return carry

        lax.fori_loop(0, group_rows // (16 * batch), norm, 0)

        def tile(i, send):
            cols = pl.ds(pl.multiple_of(i * n_tile, 128), n_tile)
            x = rows_in[...]
            gate = jnp.dot(x, wg[:, cols], preferred_element_type=f32)
            upper = jnp.dot(x, wu[:, cols], preferred_element_type=f32)
            value = gate / (1.0 + jnp.exp(-gate)) * upper
            hid[group(g), pl.ds(tile_at(i, ti), n_tile)] = value.astype(bf16)
            if send:
                send_tile(g, i)

        def loop(first, last, send):
            def body(i, carry):
                tile(i, send)
                return carry

            if last > first:
                lax.fori_loop(first, last, body, 0)

        loop(0, sent, True)
        loop(sent, tiles, False)

    def return_copy(d):
        return remote(back.at[block(d)], ret.at[block(d)], r_s.at[0], r_r.at[d - 1], {"ep": flip(me, d)})

    def relay(g, first=0, last=tiles):
        for i in range(first, last):
            for j in range(1, chips):
                hid_x(g, i, j).wait_recv()
            hid_pair(g, i).start()

    out_tile = min(256, width)

    def down(g, first=0, last=tiles, start=None, stop=True):
        for i in range(first, last):
            hid_pair(g, i).wait_recv()
        deep = pl.ds(first * tp * n_tile, (last - first) * tp * n_tile)

        def body(i, carry):
            cols = pl.ds(pl.multiple_of(i * out_tile, 128), out_tile)
            value = jnp.dot(hid[group(g), deep], wd[deep, cols], preferred_element_type=f32)
            if start is not None:
                value = value + start[:, cols]
            if stop:
                back[group(g), cols] = value.astype(bf16)
            else:
                part[:, cols] = value
            return carry

        lax.fori_loop(0, width // out_tile, body, 0)
        if stop:
            for d in members(g):
                if d > 0:
                    return_copy(d).start()
                else:
                    ret[block(0), :] = back[block(0), :]

    def piece_slots(piece):
        return pl.ds(piece[0] * group_rows, piece[1] * group_rows)

    def combine(q):
        piece, pick = pieces[q], picks[q]
        for g in range(piece[0], sum(piece)):
            for d in members(g):
                if d > 0:
                    return_copy(d).wait_recv()
        value = 0.0 if q == 0 else mix[...]
        for k in range(2):
            found = jnp.dot(pick[k], ret[piece_slots(piece), :], preferred_element_type=f32)
            value = value + found * wide(wcol[k], width)
        mix[...] = value

    for j in range(1, tp):
        meet_tp(j)
    for j in range(1, chips):
        token_copy(j).start()
    gain[:, own] = pre_ref[...]
    for j in range(1, tp):
        gain_copy(j).start()
    for g in (4, 5, 1, 2, 3, 6, 7):
        pick_own(g)
        send_own(g)
    pick_own(0)
    send_own(0)
    for k in range(2):
        column = to_column(target[k])
        wcol[k] = to_column(rw_ref[k : k + 1, :])
        for piece, pick in zip(pieces, picks):
            base = piece[0] * group_rows
            for at in range(0, pick.shape[2], 128):
                size = min(128, pick.shape[2] - at)
                lane = lax.broadcasted_iota(jnp.int32, (rows, size), 1).astype(f32)
                pick[k, :, at : at + size] = jnp.where(
                    column[:, 0:size] == lane + float(base + at), 1.0, 0.0
                ).astype(bf16)
    for j in range(1, chips):
        token_copy(j).wait_recv()
    send_rest(0)
    take(0)
    for g in (1, 6, 7, 2, 3):
        send_rest(g)
    take(4)
    for load in loads[:2]:
        load.wait()
    for j in range(1, tp):
        gain_copy(j).wait_recv()
    gate_up(0, early)
    take(5)
    take(1)
    pass_on(4)
    gate_up(1)
    pass_on(5)
    relay(0, 0, early)
    gate_up(4)
    loads[2].wait()
    if early:
        down(0, 0, early, stop=False)
    take(6)
    gate_up(5)
    relay(1)
    take(7)
    gate_up(6)
    down(1)
    relay(4)
    take(2)
    gate_up(7)
    down(4)
    relay(5)
    take(3)
    gate_up(2)
    down(5)
    relay(6)
    gate_up(3)
    send_hidden(0, early)
    down(6)
    relay(7)
    down(7)
    relay(2)
    down(2)
    combine(0)
    relay(3)
    down(3)
    relay(0, early)
    combine(1)
    down(0, early, start=part if early else None)
    combine(2)
    mixed = mix[...]
    ss_out[0] = row_sums(mixed * mixed)
    out_copies = [
        remote(ss_out.at[0], ss_out.at[j], so_s.at[0], so_r.at[j - 1], {"tp": (ti + j) % tp})
        for j in range(1, tp)
    ]
    for copy in out_copies:
        copy.start()

    def drain(ref, sem):
        remote(ref, ref, sem.at[0], so_r.at[0], {"tp": partner}).wait_send()

    later = pl.ds(cap, (n - 1) * cap)
    fresh = (groups - len(shared)) * per_group - 1
    drain(tok_x.at[:, 0 : (chips - 1) * width], t_s)
    drain(outg.at[later, 0:width], d_s)
    drain(outg.at[0 : fresh * cap, 0 : (chips - 1) * width], d_s)
    drain(back.at[later], r_s)
    drain(gain.at[:, 0 : (tp - 1) * width], g_s)
    if shared:
        drain(feats.at[0 : len(shared) * group_rows, 0 : (chips - 1) * width], fx_s)
    drain(feats.at[:, 0:side], fp_s)
    drain(hid.at[:, 0 : (chips - 1) * units], hx_s)
    drain(hid.at[:, 0 : chips * units], hp_s)
    for copy in out_copies:
        copy.wait_recv()
    total = ss_out[0]
    for j in range(1, tp):
        total = total + ss_out[j]
    scale = wide(to_column(lax.rsqrt(total / (width * tp) + epsilon)), width)
    out_ref[...] = (mixed * scale * post_ref[...]).astype(bf16)
    drain(ss_out.at[0 : tp - 1], so_s)


def on_device(
    tokens, expert_ids, route_weights, pre_gain, post_gain, gate_weight, up_weight, down_weight
):
    rows, width = tokens.shape
    n, tp = lax.axis_size("ep"), lax.axis_size("tp")
    assert gate_weight.shape[0] == 1 and expert_ids.shape[1] == 2
    capacity = max(2, rows * 2 * 5 // (4 * n))
    cap = -(-capacity // 16) * 16
    groups = 8
    assert n % groups == 0
    shared = (4, 5)
    pieces = ((4, 4), (1, 3), (0, 1))
    slots = n * cap
    chips = tp // 2
    features, units = gate_weight.shape[1:]
    hidden_all = units * tp
    tiles = units // min(256, units)
    early = tiles // 2
    group_rows = slots // groups
    dma, regular = pltpu.SemaphoreType.DMA, pltpu.SemaphoreType.REGULAR
    vmem = pl.BlockSpec(memory_space=pltpu.VMEM)
    hbm = pl.BlockSpec(memory_space=pl.ANY)
    return pl.pallas_call(
        functools.partial(kernel, n, tp, cap, groups, shared, early, pieces),
        out_shape=jax.ShapeDtypeStruct((rows, width), bf16),
        in_specs=[vmem] * 5 + [hbm] * 3,
        out_specs=vmem,
        scratch_shapes=[
            pltpu.VMEM((features, units), bf16),
            pltpu.VMEM((features, units), bf16),
            pltpu.VMEM((hidden_all, width), bf16),
            pltpu.VMEM((rows, chips * width), bf16),
            pltpu.VMEM((slots, chips * width), bf16),
            pltpu.VMEM((slots, features), bf16),
            pltpu.VMEM((group_rows, features), bf16),
            pltpu.VMEM((slots, hidden_all), bf16),
            pltpu.VMEM((group_rows, width), f32),
            pltpu.VMEM((slots, width), bf16),
            pltpu.VMEM((slots, width), bf16),
            pltpu.VMEM((1, features), f32),
            pltpu.VMEM((tp, 1, rows), f32),
            pltpu.VMEM((rows, width), f32),
            pltpu.VMEM((2, rows, 128), f32),
            *[pltpu.VMEM((2, rows, count * group_rows), bf16) for _, count in pieces],
            dma((3,)),
            regular((n - 1,)), regular((tp - 1,)),
            dma((1,)), dma((chips - 1,)),
            dma((1,)), dma((tp - 1,)), dma((1,)), dma((tp - 1,)),
            dma((1,)), dma((n - 1, chips)),
            dma((1,)), dma((groups, chips - 1)),
            dma((1,)), dma((groups,)),
            dma((1,)), dma((groups, tiles, chips - 1)),
            dma((1,)), dma((groups, tiles)),
            dma((1,)), dma((n - 1,)),
        ],
        compiler_params=pltpu.CompilerParams(
            collective_id=0, has_side_effects=True, vmem_limit_bytes=56 * 1024 * 1024
        ),
    )(
        tokens, jnp.transpose(expert_ids), jnp.transpose(route_weights),
        pre_gain.reshape(1, -1), post_gain.reshape(1, -1),
        gate_weight, up_weight, down_weight,
    )


def solution(mesh):
    return jax.shard_map(
        on_device,
        mesh=mesh,
        in_specs=(
            P("ep", "tp"),
            P("ep", None),
            P("ep", None),
            P("tp"),
            P("tp"),
            P("ep", None, "tp"),
            P("ep", None, "tp"),
            P("ep", None, "tp"),
        ),
        out_specs=P("ep", "tp"),
        check_vma=False,
    )
```

```python
import functools

import jax
import jax.numpy as jnp
from jax import lax
from jax.experimental import pallas as pl
from jax.experimental.pallas import tpu as pltpu
from jax.sharding import PartitionSpec as P

epsilon = 1e-06
MESH = pl.DeviceIdType.MESH
f32, bf16 = jnp.float32, jnp.bfloat16


def flip(index, bits):
    out, bit = index, 1
    while bit <= bits:
        if bits & bit:
            out = out + bit * (1 - 2 * ((index // bit) % 2))
        bit *= 2
    return out


def to_column(row):
    return jnp.transpose(jnp.broadcast_to(row, (128, row.shape[1])))


def wide(column, width):
    return jnp.concatenate([column] * (width // 128), axis=1)


def row_sums(values):
    part = values[:, 0:128]
    for at in range(128, values.shape[1], 128):
        part = part + values[:, at : at + 128]
    return jnp.sum(jnp.transpose(part), axis=0, keepdims=True)


def kernel(
    n, tp, cap, groups, crossed, early, pieces,
    tok_hbm, ids_hbm, rw_hbm, pre_hbm, post_hbm, wg_hbm, wu_hbm, wd_hbm,
    out_ref,
    tok_ref, ids_ref, rw_ref, pre_ref, post_ref, wg, wu, wd, outg, over, feats, rows_in, hid, part, back, ret, gain, ss_out, mix, wcol, *rest,
):
    hots, sems = rest[: len(pieces)], rest[len(pieces) :]
    (i_sem, w_sem, met_ep, met_tp, g_s, g_r, so_s, so_r, c_s, c_r, d_s, d_r, d_x, fx_s, fx_r, fp_s, fp_r,
     hx_s, hx_r, hp_s, hp_r, r_s, r_r) = sems
    me, ti = lax.axis_index("ep"), lax.axis_index("tp")
    chips = tp // 2
    chip, core = ti // 2, ti % 2
    partner = chip * 2 + (1 - core)
    rows, width = tok_ref.shape
    side = chips * width
    units = wg.shape[1]
    n_tile = min(256, units)
    tiles = units // n_tile
    per_group = n // groups
    group_rows = per_group * cap

    barrier = pltpu.get_barrier_semaphore()

    def signal(sem, where):
        pl.semaphore_signal(sem, inc=1, device_id=where, device_id_type=MESH)

    for j in range(1, tp):
        peer = (ti + j) % tp
        pl.when(peer > ti)(functools.partial(signal, barrier, {"tp": peer}))
    for d in range(1, n):
        peer = flip(me, d)
        pl.when(peer > me)(functools.partial(signal, barrier, {"ep": peer}))

    inputs = [
        pltpu.make_async_copy(src, dst, i_sem.at[i])
        for i, (src, dst) in enumerate((
            (ids_hbm, ids_ref), (tok_hbm, tok_ref), (pre_hbm, pre_ref), (rw_hbm, rw_ref),
            (post_hbm, post_ref),
        ))
    ]
    for copy in inputs:
        copy.start()

    def load_all(src, dst, sem, step, place):
        for at in range(0, dst.shape[0], step):
            pltpu.make_async_copy(
                src.at[0, pl.ds(at, step)], dst.at[pl.ds(place(at // step) * step, step)], sem
            ).start()

    def position(owner):
        return owner % 2 * chips + owner // 2

    pl.when(me + ti > 0)(lambda: pl.semaphore_wait(barrier, me + ti))
    for j in range(1, tp):
        peer = (ti + j) % tp
        pl.when(peer < ti)(functools.partial(signal, met_tp.at[tp - j - 1], {"tp": peer}))
    for d in range(1, n):
        peer = flip(me, d)
        pl.when(peer < me)(functools.partial(signal, met_ep.at[d - 1], {"ep": peer}))

    load_all(wg_hbm, wg, w_sem.at[0], width, position)
    load_all(wu_hbm, wu, w_sem.at[1], width, position)
    load_all(
        wd_hbm, wd, w_sem.at[2], n_tile, lambda at: at % tiles * tp + position(at // tiles)
    )
    loads = [
        pltpu.make_async_copy(src.at[0], dst, w_sem.at[i])
        for i, (src, dst) in enumerate(((wg_hbm, wg), (wu_hbm, wu), (wd_hbm, wd)))
    ]

    def meet_tp(j):
        pl.when((ti + j) % tp > ti)(lambda: pl.semaphore_wait(met_tp.at[j - 1], 1))

    def meet_ep(d):
        pl.when(flip(me, d) > me)(lambda: pl.semaphore_wait(met_ep.at[d - 1], 1))

    def remote(src, dst, s_sem, r_sem, where):
        return pltpu.make_async_remote_copy(
            src_ref=src, dst_ref=dst, send_sem=s_sem, recv_sem=r_sem,
            device_id=where, device_id_type=MESH,
        )

    inputs[0].wait()
    lanes = max(n, 16)
    rel = [jnp.bitwise_xor(ids_ref[k : k + 1, :], me) for k in range(2)]
    d_iota = lax.broadcasted_iota(jnp.int32, (lanes, rows), 0)
    hot = [jnp.where(rel[k] == d_iota, 1.0, 0.0).astype(f32) for k in range(2)]
    earlier = jnp.where(
        lax.broadcasted_iota(jnp.int32, (rows, rows), 0)
        < lax.broadcasted_iota(jnp.int32, (rows, rows), 1), 1.0, 0.0,
    ).astype(bf16)
    prefix = jnp.dot((hot[0] + hot[1]).astype(bf16), earlier, preferred_element_type=f32)
    target = [
        rel[k].astype(f32) * cap + jnp.sum(prefix * hot[k], axis=0, keepdims=True)
        for k in range(2)
    ]
    slot_iota = lax.broadcasted_iota(jnp.int32, (cap, rows), 0).astype(f32)

    def hop(j):
        return (chip + j) % chips

    def seg(j):
        return pl.ds(pl.multiple_of(core * side + hop(j) * width, 128), width)

    own = seg(0)
    half = pl.ds(pl.multiple_of(core * side, 128), side)

    def block(d):
        return pl.ds(d * cap, cap)

    def group(g):
        return pl.ds(g * group_rows, group_rows)

    def members(g):
        return range(g * per_group, (g + 1) * per_group)

    def gain_copy(j):
        return remote(pre_ref, gain.at[:, own], g_s.at[0], g_r.at[j - 1], {"tp": (ti + j) % tp})

    def dispatch_copy(d):
        return remote(
            outg.at[block(d)], feats.at[block(d), own], d_s.at[0], d_r.at[d - 1], {"ep": flip(me, d)}
        )

    def cross_copy(g, j):
        return remote(
            outg.at[group(g)], over.at[crossed.index(g), chip],
            c_s.at[0], c_r.at[g, j - 1], {"tp": hop(j) * 2 + core},
        )

    def forward_copy(d, j):
        g, source = d // per_group, hop(chips - j)
        return remote(
            over.at[crossed.index(g), source, pl.ds(d % per_group * cap, cap)],
            feats.at[block(d), seg(chips - j)],
            d_s.at[0], d_x.at[d - 1, j - 1], {"ep": flip(me, d)},
        )

    def feat_x(g, j):
        ref = feats.at[group(g), own]
        return remote(ref, ref, fx_s.at[0], fx_r.at[g, j - 1], {"tp": hop(j) * 2 + core})

    def feat_pair(g):
        ref = feats.at[group(g), half]
        return remote(ref, ref, fp_s.at[0], fp_r.at[g], {"tp": partner})

    def choose(d):
        base = float(d * cap)
        chosen = jnp.where(
            (target[0] == slot_iota + base) | (target[1] == slot_iota + base), 1.0, 0.0
        ).astype(bf16)
        picked = jnp.dot(chosen, tok_ref[...], preferred_element_type=f32).astype(bf16)
        if d == 0:
            feats[block(0), own] = picked
        else:
            outg[block(d), :] = picked

    def pick(g):
        for d in members(g):
            choose(d)

    def send(g):
        for d in members(g):
            if d > 0:
                meet_ep(d)
                dispatch_copy(d).start()

    def cross(g):
        for j in range(1, chips):
            cross_copy(g, j).start()

    def forward(g):
        for j in range(1, chips):
            cross_copy(g, j).wait_recv()
            for d in members(g):
                forward_copy(d, j).start()

    def share(g):
        for d in members(g):
            if d > 0:
                dispatch_copy(d).wait_recv()
        for j in range(1, chips):
            feat_x(g, j).start()

    def pass_on(g):
        for j in range(1, chips):
            if g not in crossed:
                feat_x(g, j).wait_recv()
                continue
            for d in members(g):
                if j == 1:
                    dispatch_copy(d).wait_recv()
                forward_copy(d, j).wait_recv()
        feat_pair(g).start()

    def tile_at(i, owner):
        return pl.multiple_of((i * tp + position(owner)) * n_tile, 128)

    def hid_x(g, i, j):
        ref = hid.at[group(g), pl.ds(tile_at(i, ti), n_tile)]
        return remote(ref, ref, hx_s.at[0], hx_r.at[g, i, j - 1], {"tp": hop(j) * 2 + core})

    def hid_pair(g, i):
        at = pl.multiple_of((i * tp + core * chips) * n_tile, 128)
        ref = hid.at[group(g), pl.ds(at, chips * n_tile)]
        return remote(ref, ref, hp_s.at[0], hp_r.at[g, i], {"tp": partner})

    def send_tile(g, i):
        for j in range(1, chips):
            hid_x(g, i, j).start()

    def send_hidden(g, first):
        for i in range(first, tiles):
            send_tile(g, i)

    def gate_up(g, many=1, sent=tiles):
        for at in range(g, g + many):
            feat_pair(at).wait_recv()
        count = many * group_rows
        span = pl.ds(g * group_rows, count)
        batch = max(u for u in range(1, 6) if (count // 16) % u == 0)

        def norm(i, carry):
            for u in range(batch):
                here = (i * batch + u) * 16
                here_rows = pl.ds(pl.multiple_of(g * group_rows + here, 16), 16)
                x = feats[here_rows, :].astype(f32)
                square = jnp.sum(x * x, axis=1, keepdims=True)
                x = x * lax.rsqrt(square / (width * tp) + epsilon) * gain[...]
                rows_in[pl.ds(pl.multiple_of(here, 16), 16), :] = x.astype(bf16)
            return carry

        lax.fori_loop(0, count // (16 * batch), norm, 0)

        def tile(i, send):
            cols = pl.ds(pl.multiple_of(i * n_tile, 128), n_tile)
            x = rows_in[0:count, :]
            gate = jnp.dot(x, wg[:, cols], preferred_element_type=f32)
            upper = jnp.dot(x, wu[:, cols], preferred_element_type=f32)
            value = gate / (1.0 + jnp.exp(-gate)) * upper
            hid[span, pl.ds(tile_at(i, ti), n_tile)] = value.astype(bf16)
            if send:
                for at in range(g, g + many):
                    send_tile(at, i)

        def loop(first, last, send):
            def body(i, carry):
                tile(i, send)
                return carry

            if last > first:
                lax.fori_loop(first, last, body, 0)

        loop(0, sent, True)
        loop(sent, tiles, False)

    def return_copy(d):
        return remote(back.at[block(d)], ret.at[block(d)], r_s.at[0], r_r.at[d - 1], {"ep": flip(me, d)})

    def relay(g, many=1, first=0, last=tiles):
        for i in range(first, last):
            for at in range(g, g + many):
                for j in range(1, chips):
                    hid_x(at, i, j).wait_recv()
                hid_pair(at, i).start()

    out_tile = min(256, width)

    def down(g, many=1, first=0, last=tiles, start=None, stop=True):
        for i in range(first, last):
            for at in range(g, g + many):
                hid_pair(at, i).wait_recv()
        span = pl.ds(g * group_rows, many * group_rows)
        deep = pl.ds(first * tp * n_tile, (last - first) * tp * n_tile)

        def body(i, carry):
            cols = pl.ds(pl.multiple_of(i * out_tile, 128), out_tile)
            value = jnp.dot(hid[span, deep], wd[deep, cols], preferred_element_type=f32)
            if start is not None:
                value = value + start[:, cols]
            if stop:
                back[span, cols] = value.astype(bf16)
            else:
                part[:, cols] = value
            return carry

        lax.fori_loop(0, width // out_tile, body, 0)
        if stop:
            for d in range(g * per_group, (g + many) * per_group):
                if d > 0:
                    return_copy(d).start()
                else:
                    ret[block(0), :] = back[block(0), :]

    def piece_slots(piece):
        return pl.ds(piece[0] * group_rows, piece[1] * group_rows)

    def combine(q):
        piece, hot_rows = pieces[q], hots[q]
        for g in range(piece[0], sum(piece)):
            for d in members(g):
                if d > 0:
                    return_copy(d).wait_recv()
        value = 0.0 if q == 0 else mix[...]
        for k in range(2):
            found = jnp.dot(hot_rows[k], ret[piece_slots(piece), :], preferred_element_type=f32)
            value = value + found * wide(wcol[k], width)
        mix[...] = value

    inputs[1].wait()
    pick(5)
    pick(7)
    pick(4)
    pick(0)
    pick(2)
    pick(1)
    for j in range(1, tp):
        meet_tp(j)
    send(1)
    cross(1)
    send(4)
    share(0)
    cross(2)
    pick(3)
    send(2)
    pick(6)
    cross(3)
    forward(1)
    share(4)
    send(6)
    pass_on(0)
    inputs[2].wait()
    gain[:, own] = pre_ref[...]
    for j in range(1, tp):
        gain_copy(j).start()
    pass_on(1)
    send(5)
    forward(2)
    for load in loads[:2]:
        load.wait()
    for j in range(1, tp):
        gain_copy(j).wait_recv()
    gate_up(1)
    for copy in inputs[3:]:
        copy.wait()
    for k in range(2):
        column = to_column(target[k])
        wcol[k] = to_column(rw_ref[k : k + 1, :])
        for piece, hot_rows in zip(pieces, hots):
            base = piece[0] * group_rows
            for at in range(0, hot_rows.shape[2], 128):
                size = min(128, hot_rows.shape[2] - at)
                lane = lax.broadcasted_iota(jnp.int32, (rows, size), 1).astype(f32)
                hot_rows[k, :, at : at + size] = jnp.where(
                    column[:, 0:size] == lane + float(base + at), 1.0, 0.0
                ).astype(bf16)
    gate_up(0, 1, early)
    send(7)
    share(5)
    send(3)
    relay(1)
    pass_on(4)
    relay(0, 1, 0, early)
    share(6)
    gate_up(4)
    loads[2].wait()
    down(1)
    share(7)
    pass_on(5)
    pass_on(6)
    forward(3)
    gate_up(5)
    relay(4)
    combine(0)
    gate_up(6)
    pass_on(7)
    pass_on(2)
    down(4)
    if early:
        down(0, 1, 0, early, stop=False)
    relay(5)
    pass_on(3)
    gate_up(7)
    down(5)
    relay(6)
    gate_up(2)
    down(6)
    relay(7)
    gate_up(3)
    down(7)
    relay(2)
    down(2)
    relay(3)
    send_hidden(0, early)
    down(3)
    relay(0, 1, early)
    combine(1)
    down(0, 1, early, start=part if early else None)
    combine(4)
    combine(2)
    combine(3)
    mixed = mix[...]
    ss_out[0] = row_sums(mixed * mixed)
    out_copies = [
        remote(ss_out.at[0], ss_out.at[j], so_s.at[0], so_r.at[j - 1], {"tp": (ti + j) % tp})
        for j in range(1, tp)
    ]
    for copy in out_copies:
        copy.start()
    mix[...] = mixed * post_ref[...]

    def drain(ref, sem):
        remote(ref, ref, sem.at[0], so_r.at[0], {"tp": partner}).wait_send()

    slots = n * cap
    later = pl.ds(cap, slots - cap)
    drain(outg.at[later], d_s)
    drain(back.at[later], r_s)
    drain(gain.at[:, 0 : (tp - 1) * width], g_s)
    crossing = len(crossed) * group_rows
    shared = pl.ds(0, slots - crossing)
    drain(feats.at[shared, 0 : (chips - 1) * width], fx_s)
    if crossed:
        drain(feats.at[0:crossing, 0 : (chips - 1) * width], c_s)
        drain(feats.at[0:crossing, 0 : (chips - 1) * width], d_s)
    drain(feats.at[:, 0:side], fp_s)
    drain(hid.at[:, 0 : (chips - 1) * units], hx_s)
    drain(hid.at[:, 0 : chips * units], hp_s)
    for copy in out_copies:
        copy.wait_recv()
    total = ss_out[0]
    for j in range(1, tp):
        total = total + ss_out[j]
    scale = wide(to_column(lax.rsqrt(total / (width * tp) + epsilon)), width)
    out_ref[...] = (mix[...] * scale).astype(bf16)
    drain(ss_out.at[0 : tp - 1], so_s)


def on_device(
    tokens, expert_ids, route_weights, pre_gain, post_gain, gate_weight, up_weight, down_weight
):
    rows, width = tokens.shape
    n, tp = lax.axis_size("ep"), lax.axis_size("tp")
    assert gate_weight.shape[0] == 1 and expert_ids.shape[1] == 2
    capacity = max(2, rows * 2 * 5 // (4 * n))
    cap = -(-capacity // 16) * 16
    groups = 8
    assert n % groups == 0
    crossed = (1, 2, 3)
    pieces = ((1, 1), (4, 2), (0, 1), (2, 2), (6, 2))
    slots = n * cap
    chips = tp // 2
    features, units = gate_weight.shape[1:]
    hidden_all = units * tp
    tiles = units // min(256, units)
    early = tiles // 2
    group_rows = slots // groups
    dma, regular = pltpu.SemaphoreType.DMA, pltpu.SemaphoreType.REGULAR
    vmem = pl.BlockSpec(memory_space=pltpu.VMEM)
    hbm = pl.BlockSpec(memory_space=pl.ANY)
    return pl.pallas_call(
        functools.partial(kernel, n, tp, cap, groups, crossed, early, pieces),
        out_shape=pltpu.VMEM((rows, width), bf16),
        in_specs=[hbm] * 8,
        out_specs=vmem,
        scratch_shapes=[
            pltpu.VMEM((rows, width), bf16),
            pltpu.VMEM((2, rows), jnp.int32),
            pltpu.VMEM((2, rows), f32),
            pltpu.VMEM((1, width), f32),
            pltpu.VMEM((1, width), f32),
            pltpu.VMEM((features, units), bf16),
            pltpu.VMEM((features, units), bf16),
            pltpu.VMEM((hidden_all, width), bf16),
            pltpu.VMEM((slots, width), bf16),
            pltpu.VMEM((max(1, len(crossed)), chips, group_rows, width), bf16),
            pltpu.VMEM((slots, features), bf16),
            pltpu.VMEM((2 * group_rows, features), bf16),
            pltpu.VMEM((slots, hidden_all), bf16),
            pltpu.VMEM((group_rows, width), f32),
            pltpu.VMEM((slots, width), bf16),
            pltpu.VMEM((slots, width), bf16),
            pltpu.VMEM((1, features), f32),
            pltpu.VMEM((tp, 1, rows), f32),
            pltpu.VMEM((rows, width), f32),
            pltpu.VMEM((2, rows, 128), f32),
            *[pltpu.VMEM((2, rows, count * group_rows), bf16) for _, count in pieces],
            dma((5,)), dma((3,)),
            regular((n - 1,)), regular((tp - 1,)),
            dma((1,)), dma((tp - 1,)), dma((1,)), dma((tp - 1,)),
            dma((1,)), dma((groups, chips - 1)),
            dma((1,)), dma((n - 1,)), dma((n - 1, chips - 1)),
            dma((1,)), dma((groups, chips - 1)),
            dma((1,)), dma((groups,)),
            dma((1,)), dma((groups, tiles, chips - 1)),
            dma((1,)), dma((groups, tiles)),
            dma((1,)), dma((n - 1,)),
        ],
        compiler_params=pltpu.CompilerParams(
            collective_id=0, has_side_effects=True, vmem_limit_bytes=56 * 1024 * 1024
        ),
    )(
        tokens, jnp.transpose(expert_ids), jnp.transpose(route_weights),
        pre_gain.reshape(1, -1), post_gain.reshape(1, -1),
        gate_weight, up_weight, down_weight,
    )


def solution(mesh):
    return jax.shard_map(
        on_device,
        mesh=mesh,
        in_specs=(
            P("ep", "tp"),
            P("ep", None),
            P("ep", None),
            P("tp"),
            P("tp"),
            P("ep", None, "tp"),
            P("ep", None, "tp"),
            P("ep", None, "tp"),
        ),
        out_specs=P("ep", "tp"),
        check_vma=False,
    )
```

```python
import functools

import jax
import jax.numpy as jnp
from jax import lax
from jax.experimental import pallas as pl
from jax.experimental.pallas import tpu as pltpu
from jax.sharding import PartitionSpec as P

epsilon = 1e-06
MESH = pl.DeviceIdType.MESH
f32, bf16 = jnp.float32, jnp.bfloat16


def flip(index, bits):
    out, bit = index, 1
    while bit <= bits:
        if bits & bit:
            out = out + bit * (1 - 2 * ((index // bit) % 2))
        bit *= 2
    return out


def to_column(row):
    return jnp.transpose(jnp.broadcast_to(row, (128, row.shape[1])))


def wide(column, width):
    return jnp.concatenate([column] * (width // 128), axis=1)


def row_sums(values):
    part = values[:, 0:128]
    for at in range(128, values.shape[1], 128):
        part = part + values[:, at : at + 128]
    return jnp.sum(jnp.transpose(part), axis=0, keepdims=True)


def kernel(
    n, tp, cap, groups, crossed, early, pieces,
    tok_hbm, ids_hbm, rw_hbm, pre_hbm, post_hbm, wg_hbm, wu_hbm, wd_hbm,
    out_ref,
    tok_ref, ids_ref, rw_ref, pre_ref, post_ref, wg, wu, wd, outg, over, feats, rows_in, hid, part, back, ret, gain, ss_out, mix, wcol, *rest,
):
    hots, sems = rest[: len(pieces)], rest[len(pieces) :]
    (i_sem, w_sem, met_ep, met_tp, g_s, g_r, so_s, so_r, c_s, c_r, d_s, d_r, d_x, fx_s, fx_r, fp_s, fp_r,
     hx_s, hx_r, hp_s, hp_r, r_s, r_r) = sems
    me, ti = lax.axis_index("ep"), lax.axis_index("tp")
    chips = tp // 2
    chip, core = ti // 2, ti % 2
    partner = chip * 2 + (1 - core)
    rows, width = tok_ref.shape
    side = chips * width
    units = wg.shape[1]
    n_tile = min(256, units)
    tiles = units // n_tile
    per_group = n // groups
    group_rows = per_group * cap

    barrier = pltpu.get_barrier_semaphore()

    def signal(sem, where):
        pl.semaphore_signal(sem, inc=1, device_id=where, device_id_type=MESH)

    for j in range(1, tp):
        peer = (ti + j) % tp
        pl.when(peer > ti)(functools.partial(signal, barrier, {"tp": peer}))
    for d in range(1, n):
        peer = flip(me, d)
        pl.when(peer > me)(functools.partial(signal, barrier, {"ep": peer}))

    inputs = [
        pltpu.make_async_copy(src, dst, i_sem.at[i])
        for i, (src, dst) in enumerate((
            (ids_hbm, ids_ref), (tok_hbm, tok_ref), (pre_hbm, pre_ref), (rw_hbm, rw_ref),
            (post_hbm, post_ref),
        ))
    ]
    for copy in inputs:
        copy.start()

    def load_all(src, dst, sem, step, place):
        for at in range(0, dst.shape[0], step):
            pltpu.make_async_copy(
                src.at[0, pl.ds(at, step)], dst.at[pl.ds(place(at // step) * step, step)], sem
            ).start()

    def position(owner):
        return owner % 2 * chips + owner // 2

    pl.when(me + ti > 0)(lambda: pl.semaphore_wait(barrier, me + ti))
    for j in range(1, tp):
        peer = (ti + j) % tp
        pl.when(peer < ti)(functools.partial(signal, met_tp.at[tp - j - 1], {"tp": peer}))
    for d in range(1, n):
        peer = flip(me, d)
        pl.when(peer < me)(functools.partial(signal, met_ep.at[d - 1], {"ep": peer}))

    load_all(wg_hbm, wg, w_sem.at[0], width, position)
    load_all(wu_hbm, wu, w_sem.at[1], width, position)
    load_all(
        wd_hbm, wd, w_sem.at[2], n_tile, lambda at: at % tiles * tp + position(at // tiles)
    )
    loads = [
        pltpu.make_async_copy(src.at[0], dst, w_sem.at[i])
        for i, (src, dst) in enumerate(((wg_hbm, wg), (wu_hbm, wu), (wd_hbm, wd)))
    ]

    def meet_tp(j):
        pl.when((ti + j) % tp > ti)(lambda: pl.semaphore_wait(met_tp.at[j - 1], 1))

    def meet_ep(d):
        pl.when(flip(me, d) > me)(lambda: pl.semaphore_wait(met_ep.at[d - 1], 1))

    def remote(src, dst, s_sem, r_sem, where):
        return pltpu.make_async_remote_copy(
            src_ref=src, dst_ref=dst, send_sem=s_sem, recv_sem=r_sem,
            device_id=where, device_id_type=MESH,
        )

    inputs[0].wait()
    lanes = max(n, 16)
    rel = [jnp.bitwise_xor(ids_ref[k : k + 1, :], me) for k in range(2)]
    d_iota = lax.broadcasted_iota(jnp.int32, (lanes, rows), 0)
    hot = [jnp.where(rel[k] == d_iota, 1.0, 0.0).astype(f32) for k in range(2)]
    earlier = jnp.where(
        lax.broadcasted_iota(jnp.int32, (rows, rows), 0)
        < lax.broadcasted_iota(jnp.int32, (rows, rows), 1), 1.0, 0.0,
    ).astype(bf16)
    prefix = jnp.dot((hot[0] + hot[1]).astype(bf16), earlier, preferred_element_type=f32)
    target = [
        rel[k].astype(f32) * cap + jnp.sum(prefix * hot[k], axis=0, keepdims=True)
        for k in range(2)
    ]
    slot_iota = lax.broadcasted_iota(jnp.int32, (cap, rows), 0).astype(f32)

    def hop(j):
        return (chip + j) % chips

    def seg(j):
        return pl.ds(pl.multiple_of(core * side + hop(j) * width, 128), width)

    own = seg(0)
    half = pl.ds(pl.multiple_of(core * side, 128), side)

    def block(d):
        return pl.ds(d * cap, cap)

    def group(g):
        return pl.ds(g * group_rows, group_rows)

    def members(g):
        return range(g * per_group, (g + 1) * per_group)

    def gain_copy(j):
        return remote(pre_ref, gain.at[:, own], g_s.at[0], g_r.at[j - 1], {"tp": (ti + j) % tp})

    def dispatch_copy(d):
        return remote(
            outg.at[block(d)], feats.at[block(d), own], d_s.at[0], d_r.at[d - 1], {"ep": flip(me, d)}
        )

    def cross_copy(g, j):
        return remote(
            outg.at[group(g)], over.at[crossed.index(g), chip],
            c_s.at[0], c_r.at[g, j - 1], {"tp": hop(j) * 2 + core},
        )

    def forward_copy(d, j):
        g, source = d // per_group, hop(chips - j)
        return remote(
            over.at[crossed.index(g), source, pl.ds(d % per_group * cap, cap)],
            feats.at[block(d), seg(chips - j)],
            d_s.at[0], d_x.at[d - 1, j - 1], {"ep": flip(me, d)},
        )

    def feat_x(g, j):
        ref = feats.at[group(g), own]
        return remote(ref, ref, fx_s.at[0], fx_r.at[g, j - 1], {"tp": hop(j) * 2 + core})

    def feat_pair(g):
        ref = feats.at[group(g), half]
        return remote(ref, ref, fp_s.at[0], fp_r.at[g], {"tp": partner})

    def choose(d):
        base = float(d * cap)
        chosen = jnp.where(
            (target[0] == slot_iota + base) | (target[1] == slot_iota + base), 1.0, 0.0
        ).astype(bf16)
        picked = jnp.dot(chosen, tok_ref[...], preferred_element_type=f32).astype(bf16)
        if d == 0:
            feats[block(0), own] = picked
        else:
            outg[block(d), :] = picked

    def pick(g):
        for d in members(g):
            choose(d)

    def send(g):
        for d in members(g):
            if d > 0:
                meet_ep(d)
                dispatch_copy(d).start()

    def cross(g):
        for j in range(1, chips):
            cross_copy(g, j).start()

    def forward(g):
        for j in range(1, chips):
            cross_copy(g, j).wait_recv()
            for d in members(g):
                forward_copy(d, j).start()

    def share(g):
        for d in members(g):
            if d > 0:
                dispatch_copy(d).wait_recv()
        for j in range(1, chips):
            feat_x(g, j).start()

    def pass_on(g):
        for j in range(1, chips):
            if g not in crossed:
                feat_x(g, j).wait_recv()
                continue
            for d in members(g):
                if j == 1:
                    dispatch_copy(d).wait_recv()
                forward_copy(d, j).wait_recv()
        feat_pair(g).start()

    def tile_at(i, owner):
        return pl.multiple_of((i * tp + position(owner)) * n_tile, 128)

    def hid_x(g, i, j):
        ref = hid.at[group(g), pl.ds(tile_at(i, ti), n_tile)]
        return remote(ref, ref, hx_s.at[0], hx_r.at[g, i, j - 1], {"tp": hop(j) * 2 + core})

    def hid_pair(g, i):
        at = pl.multiple_of((i * tp + core * chips) * n_tile, 128)
        ref = hid.at[group(g), pl.ds(at, chips * n_tile)]
        return remote(ref, ref, hp_s.at[0], hp_r.at[g, i], {"tp": partner})

    def send_tile(g, i):
        for j in range(1, chips):
            hid_x(g, i, j).start()

    def send_hidden(g, first):
        for i in range(first, tiles):
            send_tile(g, i)

    def gate_up(g, many=1, sent=tiles):
        for at in range(g, g + many):
            feat_pair(at).wait_recv()
        count = many * group_rows
        span = pl.ds(g * group_rows, count)
        batch = max(u for u in range(1, 6) if (count // 16) % u == 0)

        def norm(i, carry):
            for u in range(batch):
                here = (i * batch + u) * 16
                here_rows = pl.ds(pl.multiple_of(g * group_rows + here, 16), 16)
                x = feats[here_rows, :].astype(f32)
                square = jnp.sum(x * x, axis=1, keepdims=True)
                x = x * lax.rsqrt(square / (width * tp) + epsilon) * gain[...]
                rows_in[pl.ds(pl.multiple_of(here, 16), 16), :] = x.astype(bf16)
            return carry

        lax.fori_loop(0, count // (16 * batch), norm, 0)

        def tile(i, send):
            cols = pl.ds(pl.multiple_of(i * n_tile, 128), n_tile)
            x = rows_in[0:count, :]
            gate = jnp.dot(x, wg[:, cols], preferred_element_type=f32)
            upper = jnp.dot(x, wu[:, cols], preferred_element_type=f32)
            value = gate / (1.0 + jnp.exp(-gate)) * upper
            hid[span, pl.ds(tile_at(i, ti), n_tile)] = value.astype(bf16)
            if send:
                for at in range(g, g + many):
                    send_tile(at, i)

        def loop(first, last, send):
            def body(i, carry):
                tile(i, send)
                return carry

            if last > first:
                lax.fori_loop(first, last, body, 0)

        loop(0, sent, True)
        loop(sent, tiles, False)

    def return_copy(d):
        return remote(back.at[block(d)], ret.at[block(d)], r_s.at[0], r_r.at[d - 1], {"ep": flip(me, d)})

    def relay(g, many=1, first=0, last=tiles):
        for i in range(first, last):
            for at in range(g, g + many):
                for j in range(1, chips):
                    hid_x(at, i, j).wait_recv()
                hid_pair(at, i).start()

    out_tile = min(256, width)

    def down(g, many=1, first=0, last=tiles, start=None, stop=True):
        for i in range(first, last):
            for at in range(g, g + many):
                hid_pair(at, i).wait_recv()
        span = pl.ds(g * group_rows, many * group_rows)
        deep = pl.ds(first * tp * n_tile, (last - first) * tp * n_tile)

        def body(i, carry):
            cols = pl.ds(pl.multiple_of(i * out_tile, 128), out_tile)
            value = jnp.dot(hid[span, deep], wd[deep, cols], preferred_element_type=f32)
            if start is not None:
                value = value + start[:, cols]
            if stop:
                back[span, cols] = value.astype(bf16)
            else:
                part[:, cols] = value
            return carry

        lax.fori_loop(0, width // out_tile, body, 0)
        if stop:
            for d in range(g * per_group, (g + many) * per_group):
                if d > 0:
                    return_copy(d).start()
                else:
                    ret[block(0), :] = back[block(0), :]

    def piece_slots(piece):
        return pl.ds(piece[0] * group_rows, piece[1] * group_rows)

    def combine(q):
        piece, hot_rows = pieces[q], hots[q]
        for g in range(piece[0], sum(piece)):
            for d in members(g):
                if d > 0:
                    return_copy(d).wait_recv()
        value = 0.0 if q == 0 else mix[...]
        for k in range(2):
            found = jnp.dot(hot_rows[k], ret[piece_slots(piece), :], preferred_element_type=f32)
            value = value + found * wide(wcol[k], width)
        mix[...] = value

    inputs[1].wait()
    pick(4)
    pick(7)
    pick(0)
    pick(1)
    pick(6)
    pick(2)
    for j in range(1, tp):
        meet_tp(j)
    cross(1)
    share(0)
    send(4)
    pick(5)
    send(1)
    cross(2)
    pick(3)
    forward(1)
    cross(3)
    send(2)
    inputs[2].wait()
    gain[:, own] = pre_ref[...]
    for j in range(1, tp):
        gain_copy(j).start()
    send(6)
    share(4)
    send(5)
    pass_on(0)
    pass_on(1)
    for load in loads[:2]:
        load.wait()
    for j in range(1, tp):
        gain_copy(j).wait_recv()
    gate_up(1)
    send(3)
    send(7)
    for copy in inputs[3:]:
        copy.wait()
    for k in range(2):
        column = to_column(target[k])
        wcol[k] = to_column(rw_ref[k : k + 1, :])
        for piece, hot_rows in zip(pieces, hots):
            base = piece[0] * group_rows
            for at in range(0, hot_rows.shape[2], 128):
                size = min(128, hot_rows.shape[2] - at)
                lane = lax.broadcasted_iota(jnp.int32, (rows, size), 1).astype(f32)
                hot_rows[k, :, at : at + size] = jnp.where(
                    column[:, 0:size] == lane + float(base + at), 1.0, 0.0
                ).astype(bf16)
    gate_up(0, 1, early)
    share(5)
    pass_on(4)
    relay(1)
    forward(2)
    relay(0, 1, 0, early)
    share(6)
    gate_up(4)
    loads[2].wait()
    down(1)
    if early:
        down(0, 1, 0, early, stop=False)
    pass_on(5)
    share(7)
    pass_on(6)
    gate_up(5)
    forward(3)
    gate_up(6)
    combine(0)
    pass_on(2)
    relay(4)
    pass_on(7)
    down(4)
    relay(5)
    pass_on(3)
    gate_up(7)
    down(5)
    relay(6)
    gate_up(2)
    down(6)
    relay(7)
    gate_up(3)
    down(7)
    relay(2)
    send_hidden(0, early)
    down(2)
    relay(3)
    down(3)
    relay(0, 1, early)
    combine(1)
    down(0, 1, early, start=part if early else None)
    combine(4)
    combine(2)
    combine(3)
    mixed = mix[...]
    ss_out[0] = row_sums(mixed * mixed)
    out_copies = [
        remote(ss_out.at[0], ss_out.at[j], so_s.at[0], so_r.at[j - 1], {"tp": (ti + j) % tp})
        for j in range(1, tp)
    ]
    for copy in out_copies:
        copy.start()
    mix[...] = mixed * post_ref[...]

    def drain(ref, sem):
        remote(ref, ref, sem.at[0], so_r.at[0], {"tp": partner}).wait_send()

    slots = n * cap
    later = pl.ds(cap, slots - cap)
    drain(outg.at[later], d_s)
    drain(back.at[later], r_s)
    drain(gain.at[:, 0 : (tp - 1) * width], g_s)
    crossing = len(crossed) * group_rows
    shared = pl.ds(0, slots - crossing)
    drain(feats.at[shared, 0 : (chips - 1) * width], fx_s)
    if crossed:
        drain(feats.at[0:crossing, 0 : (chips - 1) * width], c_s)
        drain(feats.at[0:crossing, 0 : (chips - 1) * width], d_s)
    drain(feats.at[:, 0:side], fp_s)
    drain(hid.at[:, 0 : (chips - 1) * units], hx_s)
    drain(hid.at[:, 0 : chips * units], hp_s)
    for copy in out_copies:
        copy.wait_recv()
    total = ss_out[0]
    for j in range(1, tp):
        total = total + ss_out[j]
    scale = wide(to_column(lax.rsqrt(total / (width * tp) + epsilon)), width)
    out_ref[...] = (mix[...] * scale).astype(bf16)
    drain(ss_out.at[0 : tp - 1], so_s)


def on_device(
    tokens, expert_ids, route_weights, pre_gain, post_gain, gate_weight, up_weight, down_weight
):
    rows, width = tokens.shape
    n, tp = lax.axis_size("ep"), lax.axis_size("tp")
    assert gate_weight.shape[0] == 1 and expert_ids.shape[1] == 2
    capacity = max(2, rows * 2 * 5 // (4 * n))
    cap = -(-capacity // 16) * 16
    groups = 8
    assert n % groups == 0
    crossed = (1, 2, 3)
    pieces = ((1, 1), (4, 2), (0, 1), (2, 2), (6, 2))
    slots = n * cap
    chips = tp // 2
    features, units = gate_weight.shape[1:]
    hidden_all = units * tp
    tiles = units // min(256, units)
    early = tiles // 2
    group_rows = slots // groups
    dma, regular = pltpu.SemaphoreType.DMA, pltpu.SemaphoreType.REGULAR
    vmem = pl.BlockSpec(memory_space=pltpu.VMEM)
    hbm = pl.BlockSpec(memory_space=pl.ANY)
    return pl.pallas_call(
        functools.partial(kernel, n, tp, cap, groups, crossed, early, pieces),
        out_shape=pltpu.VMEM((rows, width), bf16),
        in_specs=[hbm] * 8,
        out_specs=vmem,
        scratch_shapes=[
            pltpu.VMEM((rows, width), bf16),
            pltpu.VMEM((2, rows), jnp.int32),
            pltpu.VMEM((2, rows), f32),
            pltpu.VMEM((1, width), f32),
            pltpu.VMEM((1, width), f32),
            pltpu.VMEM((features, units), bf16),
            pltpu.VMEM((features, units), bf16),
            pltpu.VMEM((hidden_all, width), bf16),
            pltpu.VMEM((slots, width), bf16),
            pltpu.VMEM((max(1, len(crossed)), chips, group_rows, width), bf16),
            pltpu.VMEM((slots, features), bf16),
            pltpu.VMEM((2 * group_rows, features), bf16),
            pltpu.VMEM((slots, hidden_all), bf16),
            pltpu.VMEM((group_rows, width), f32),
            pltpu.VMEM((slots, width), bf16),
            pltpu.VMEM((slots, width), bf16),
            pltpu.VMEM((1, features), f32),
            pltpu.VMEM((tp, 1, rows), f32),
            pltpu.VMEM((rows, width), f32),
            pltpu.VMEM((2, rows, 128), f32),
            *[pltpu.VMEM((2, rows, count * group_rows), bf16) for _, count in pieces],
            dma((5,)), dma((3,)),
            regular((n - 1,)), regular((tp - 1,)),
            dma((1,)), dma((tp - 1,)), dma((1,)), dma((tp - 1,)),
            dma((1,)), dma((groups, chips - 1)),
            dma((1,)), dma((n - 1,)), dma((n - 1, chips - 1)),
            dma((1,)), dma((groups, chips - 1)),
            dma((1,)), dma((groups,)),
            dma((1,)), dma((groups, tiles, chips - 1)),
            dma((1,)), dma((groups, tiles)),
            dma((1,)), dma((n - 1,)),
        ],
        compiler_params=pltpu.CompilerParams(
            collective_id=0, has_side_effects=True, vmem_limit_bytes=56 * 1024 * 1024
        ),
    )(
        tokens, jnp.transpose(expert_ids), jnp.transpose(route_weights),
        pre_gain.reshape(1, -1), post_gain.reshape(1, -1),
        gate_weight, up_weight, down_weight,
    )


def solution(mesh):
    return jax.shard_map(
        on_device,
        mesh=mesh,
        in_specs=(
            P("ep", "tp"),
            P("ep", None),
            P("ep", None),
            P("tp"),
            P("tp"),
            P("ep", None, "tp"),
            P("ep", None, "tp"),
            P("ep", None, "tp"),
        ),
        out_specs=P("ep", "tp"),
        check_vma=False,
    )
```
